32 devices in a mesh: sp: 4 (over z), fs: 4 (over y, x), tp: 2 (over core).
Axes of the slice: x: 2, y: 2, z: 4, core: 2. Of those that a mesh axis runs over, the one named last changes fastest.
Arguments:
- statespace_input: bfloat16 [4, 1536, 2048], P('fs', 'sp', 'tp'), may hold values from -6 to 6
- output_gate_input: bfloat16 [4, 1536, 2048], P('fs', 'sp', 'tp'), may hold values from -6 to 6
- state_input_projection: bfloat16 [4, 1536, 512], P('fs', 'sp', 'tp'), may hold values from -6 to 6
- state_output_projection: bfloat16 [4, 1536, 512], P('fs', 'sp', 'tp'), may hold values from -6 to 6
- step_size_input: bfloat16 [4, 1536, 32], P('fs', 'sp', 'tp'), may hold values from -5 to 5
- added_log_decay: float32 [4, 1536, 32], P('fs', 'sp', 'tp'), may hold values from -0.7 to 0
- logarithm_rates: float32 [32], replicated, may hold values from -20 to -2.9
- head_channel_taps: bfloat16 [4, 2048], replicated, may hold values from -3 to 3
- input_projection_taps: bfloat16 [4, 512], replicated, may hold values from -3 to 3
- output_projection_taps: bfloat16 [4, 512], replicated, may hold values from -3 to 3
- input_projection_bias: bfloat16 [512], replicated, may hold values from -0.59765625 to -0.19921875
- group_norm_gain: bfloat16 [2048], replicated, may hold values from 0.099609375 to 1.8984375
- pooling_input: bfloat16 [4, 1536, 1024], P('fs', 'sp', 'tp'), may hold values from -6 to 6
- pooling_group_weight: bfloat16 [4, 256, 256], replicated, may hold values from -0.375 to 0.375
- pooling_channel_scale: bfloat16 [1024], replicated, may hold values from 0.099609375 to 1.8984375
- statespace_output_weight: bfloat16 [2048, 4096], P('tp', ('sp', 'fs')), may hold values from -8 to 8
- pooling_output_weight: bfloat16 [1024, 4096], P('tp', ('sp', 'fs')), may hold values from -8 to 8
- output_norm_gain: bfloat16 [4096], replicated, may hold values from 0.099609375 to 1.8984375
Outputs:
- output: bfloat16 [4, 1536, 4096], P('fs', 'sp', 'tp')
The draws below stay inside these ranges and needn't reach their ends.
All inputs are finite; a program needn't handle non-finite values.
Results may differ from the reference program's by a relative error of at most 0.02.
Values may be sent and summed in bfloat16 or wider, within the bound.
A program may use at most 128 MiB of HBM per device.

```python
import jax
import jax.numpy as jnp
from jax import lax

D = 4096
HEADS = 32
HEAD_DIM = 64
GROUPS = 4
STATE = 128
CONV = 4
BLOCK = 128
POOL_GROUPS = 4
POOL_GROUP = 256
TOK_DEV = 384
INNER = 2048
POOL = 1024
SEQUENCE_TOKENS = 1536
SEQS = 4
N_TP = 2


def draw_step_size_input(key, part):
    noise_key, level_key = jax.random.split(jax.random.fold_in(key, 3))
    blocks = SEQUENCE_TOKENS // TOK_DEV
    levels = jax.random.uniform(level_key, (SEQS, blocks, 1, HEADS), jnp.float32, -1.2, 1.2)
    noise_part = 0.7 * jax.random.normal(noise_key, (SEQS, blocks, TOK_DEV, HEADS), jnp.float32)
    values = jnp.clip(levels + noise_part, -5.0, 5.0)
    return values.reshape(SEQS, SEQUENCE_TOKENS, HEADS).astype(jnp.bfloat16)


def draw_logarithm_rates(key, part):
    order_key, fast_key, slow_key = jax.random.split(jax.random.fold_in(key, 5), 3)
    shuffled = jax.random.permutation(order_key, HEADS)
    fast_heads = shuffled < HEADS // 2
    fast_rate = jnp.exp(jax.random.uniform(fast_key, (HEADS,), jnp.float32, jnp.log(0.02), jnp.log(0.05)))
    slow_rate = jax.random.uniform(slow_key, (HEADS,), jnp.float32, 0.15, 0.45) / SEQUENCE_TOKENS
    return jnp.log(jnp.where(fast_heads, fast_rate, slow_rate)).astype(jnp.float32)


def draw_added_log_decay(key, part):
    first_key, second_key, size_key = jax.random.split(jax.random.fold_in(key, 9), 3)
    half_len = SEQUENCE_TOKENS // 2
    first_position = jax.random.randint(first_key, (SEQS, 1), 0, half_len)
    second_position = jax.random.randint(second_key, (SEQS, 1), 0, SEQUENCE_TOKENS - half_len) + half_len
    spike_positions = jnp.concatenate([first_position, second_position], axis=1)
    retained_fraction = jax.random.uniform(size_key, (SEQS, 2, HEADS), jnp.float32, 0.5, 0.8)
    spike_hits = (jnp.arange(SEQUENCE_TOKENS, dtype=jnp.int32)[None, :, None] == spike_positions[:, None, :]).astype(jnp.float32)
    return jnp.einsum('lga,lab->lgb', spike_hits, jnp.log(retained_fraction)).astype(jnp.float32)


def column_scales(key):
    noise_part = jnp.clip(jax.random.normal(jax.random.fold_in(key, 17), (D,), jnp.float32), -2.0, 2.0)
    column_ramp = jnp.arange(D, dtype=jnp.float32) / D
    log_scale = jnp.log(0.3) + jnp.log(10.0) * column_ramp
    return jnp.exp(log_scale + 0.3 * noise_part)


def draw_statespace_output_weight(key, part):
    values = jnp.clip(jax.random.normal(jax.random.fold_in(key, 21), (INNER, D), jnp.float32), -6.0, 6.0)
    scaled = values * column_scales(key)[None, :] / jnp.sqrt(jnp.float32(INNER + POOL))
    return jnp.clip(scaled, -8.0, 8.0).astype(jnp.bfloat16)


def draw_pooling_output_weight(key, part):
    values = jnp.clip(jax.random.normal(jax.random.fold_in(key, 23), (POOL, D), jnp.float32), -6.0, 6.0)
    scaled = values * column_scales(key)[None, :] / jnp.sqrt(jnp.float32(INNER + POOL))
    return jnp.clip(scaled, -8.0, 8.0).astype(jnp.bfloat16)


def steps_of(key, dims, cuts, smallest, high):
    level = 1.0
    for axis_at, shards_of in cuts:
        draws = jax.random.uniform(jax.random.fold_in(jax.random.fold_in(key, 6), axis_at), (shards_of,), jnp.float32, smallest / len(cuts), high / len(cuts))
        level = level * jnp.repeat(jnp.exp(draws), dims[axis_at] // shards_of).reshape((-1,) + (1,) * (len(dims) - 1 - axis_at))
    return level


def noise(own_key, shape, width, most, cuts=(), kind=jnp.bfloat16):
    loudness = steps_of(own_key, shape, cuts, -0.22, 0.18) if cuts else 1.0
    entries = jax.random.normal(own_key, shape, jnp.float32) * width * loudness
    return jnp.minimum(jnp.maximum(entries, -most), most).astype(kind)


def setup_inputs(seed: int = 0) -> dict:
    arg_keys = jax.random.split(jax.random.key(seed), 19)
    statespace_input = noise(arg_keys[0], (SEQS, SEQUENCE_TOKENS, INNER), 1.0, 6.0, ((0, 4), (1, 4), (2, 2)))
    output_gate_input = noise(arg_keys[1], (SEQS, SEQUENCE_TOKENS, INNER), 1.0, 6.0, ((0, 4), (1, 4), (2, 2)))
    state_input_projection = noise(arg_keys[2], (SEQS, SEQUENCE_TOKENS, GROUPS * STATE), 1.0, 6.0, ((0, 4), (1, 4), (2, 2)))
    state_output_projection = noise(arg_keys[3], (SEQS, SEQUENCE_TOKENS, GROUPS * STATE), 1.0, 6.0, ((0, 4), (1, 4), (2, 2)))
    step_size_input = draw_step_size_input(jax.random.fold_in(arg_keys[18], 71), 0)
    added_log_decay = draw_added_log_decay(jax.random.fold_in(arg_keys[18], 71), 0)
    logarithm_rates = draw_logarithm_rates(jax.random.fold_in(arg_keys[18], 71), 0)
    head_channel_taps = noise(arg_keys[7], (CONV, INNER), CONV ** -0.5, 3.0)
    input_projection_taps = noise(arg_keys[8], (CONV, GROUPS * STATE), CONV ** -0.5, 3.0)
    output_projection_taps = noise(arg_keys[9], (CONV, GROUPS * STATE), CONV ** -0.5, 3.0)
    input_projection_bias = jnp.clip(jax.random.uniform(arg_keys[10], (GROUPS * STATE,), jnp.float32, -0.59765625, -0.19921875), -0.59765625, -0.19921875).astype(jnp.bfloat16)
    group_norm_gain = jnp.clip(1.0 + 0.18 * jax.random.normal(arg_keys[11], (INNER,), jnp.float32), 0.099609375, 1.8984375).astype(jnp.bfloat16)
    pooling_input = noise(arg_keys[12], (SEQS, SEQUENCE_TOKENS, POOL), 1.0, 6.0, ((0, 4), (1, 4), (2, 2)))
    pooling_group_weight = noise(arg_keys[13], (POOL_GROUPS, POOL_GROUP, POOL_GROUP), POOL_GROUP ** -0.5, 0.375)
    pooling_channel_scale = jnp.clip(1.0 + 0.18 * jax.random.normal(arg_keys[14], (POOL,), jnp.float32), 0.099609375, 1.8984375).astype(jnp.bfloat16)
    statespace_output_weight = draw_statespace_output_weight(jax.random.fold_in(arg_keys[18], 71), 0)
    pooling_output_weight = draw_pooling_output_weight(jax.random.fold_in(arg_keys[18], 71), 0)
    output_norm_gain = jnp.clip(1.0 + 0.18 * jax.random.normal(arg_keys[17], (D,), jnp.float32), 0.099609375, 1.8984375).astype(jnp.bfloat16)
    return {"statespace_input": statespace_input, "output_gate_input": output_gate_input, "state_input_projection": state_input_projection, "state_output_projection": state_output_projection, "step_size_input": step_size_input, "added_log_decay": added_log_decay, "logarithm_rates": logarithm_rates, "head_channel_taps": head_channel_taps, "input_projection_taps": input_projection_taps, "output_projection_taps": output_projection_taps, "input_projection_bias": input_projection_bias, "group_norm_gain": group_norm_gain, "pooling_input": pooling_input, "pooling_group_weight": pooling_group_weight, "pooling_channel_scale": pooling_channel_scale, "statespace_output_weight": statespace_output_weight, "pooling_output_weight": pooling_output_weight, "output_norm_gain": output_norm_gain}


eps = 1e-06

def causal_taps(input_rows, prior_rows, tap_weights, offset_bias):
    padded = jnp.concatenate([prior_rows, input_rows], axis=1).astype(jnp.float32)
    tok_rows = input_rows.shape[1]
    running = jnp.zeros(input_rows.shape, jnp.float32) + offset_bias
    for tap_index in range(tap_weights.shape[0]):
        running = running + tap_weights[tap_index].astype(jnp.float32) * padded[:, tap_index:tap_index + tok_rows]
    return jax.nn.silu(running).astype(jnp.bfloat16)

def pool_mix(input_rows, prior_rows, positions, group_ids, pooling_group_weight, pooling_channel_scale):
    tail_rows = prior_rows.shape[1]
    tok_rows = input_rows.shape[1]
    padded = jnp.concatenate([prior_rows, input_rows], axis=1).astype(jnp.float32)
    window_reach = jnp.left_shift(jnp.int32(2), group_ids)
    running = jnp.zeros(input_rows.shape, jnp.float32)
    for offset_back in range(tail_rows + 1):
        start_row = tail_rows - offset_back
        running = running + padded[:, start_row:start_row + tok_rows] * (offset_back < window_reach).astype(jnp.float32)
    window_count = jnp.minimum(positions[:, None] + 1.0, window_reach.astype(jnp.float32)[None, :])
    pooled = (running / window_count - input_rows.astype(jnp.float32)).astype(jnp.bfloat16)
    grouped = pooled.reshape(input_rows.shape[:2] + (pooling_group_weight.shape[0], pooling_group_weight.shape[1]))
    mixed = jnp.einsum('slgc,gcd->slgd', grouped.astype(jnp.float32), pooling_group_weight.astype(jnp.float32))
    return (mixed.reshape(input_rows.shape) * pooling_channel_scale.astype(jnp.float32)).astype(jnp.bfloat16)

def reference(statespace_input, output_gate_input, state_input_projection, state_output_projection, step_size_input, added_log_decay, logarithm_rates, head_channel_taps, input_projection_taps, output_projection_taps, input_projection_bias, group_norm_gain, pooling_input, pooling_group_weight, pooling_channel_scale, statespace_output_weight, pooling_output_weight, output_norm_gain):
    seq_count = statespace_input.shape[0]
    number_of_blocks = SEQUENCE_TOKENS // BLOCK
    per_group = HEADS // GROUPS
    pool_tail = 2 ** POOL_GROUPS - 1

    def block_split(source):
        return jnp.moveaxis(source.reshape((seq_count, number_of_blocks, BLOCK) + source.shape[2:]), 1, 0)
    mixer_inputs = (block_split(statespace_input), block_split(output_gate_input), block_split(state_input_projection), block_split(state_output_projection), block_split(step_size_input), block_split(added_log_decay), block_split(pooling_input), jnp.arange(number_of_blocks, dtype=jnp.int32))
    group_ids = jnp.arange(POOL, dtype=jnp.int32) // POOL_GROUP
    head_decay_rates = jnp.exp(logarithm_rates)
    causal = jnp.arange(BLOCK)[:, None] >= jnp.arange(BLOCK)[None, :]
    share_ssd = INNER // N_TP
    share_pool = POOL // N_TP

    def advance(carried, current_inputs):
        state_now, prior_x, prior_b, prior_c, prior_pool = carried
        head_channel_rows, output_gate_rows, input_projection_rows, output_projection_rows, step_size_rows, decay_spikes, pooling_rows, current_block_index = current_inputs
        x_conv = causal_taps(head_channel_rows, prior_x, head_channel_taps, 0.0)
        b_conv = causal_taps(input_projection_rows, prior_b, input_projection_taps, input_projection_bias.astype(jnp.float32))
        c_conv = causal_taps(output_projection_rows, prior_c, output_projection_taps, 0.0)
        discrete_step_size = jax.nn.softplus(step_size_rows.astype(jnp.float32))
        cumulative_decay = jnp.cumsum(-discrete_step_size * head_decay_rates + decay_spikes, axis=1)
        cumulative_decay = cumulative_decay.reshape(seq_count, BLOCK, GROUPS, per_group)
        cum_t = cumulative_decay.transpose(0, 2, 3, 1)
        step_t = discrete_step_size.reshape(seq_count, BLOCK, GROUPS, per_group).transpose(0, 2, 3, 1)
        heads_x = x_conv.reshape(seq_count, BLOCK, GROUPS, per_group, HEAD_DIM).astype(jnp.float32)
        group_b = b_conv.reshape(seq_count, BLOCK, GROUPS, STATE).astype(jnp.float32)
        group_c = c_conv.reshape(seq_count, BLOCK, GROUPS, STATE).astype(jnp.float32)
        scores = jnp.einsum('stgn,sugn->sgtu', group_c, group_b)
        decay_gap = cum_t[..., :, None] - cum_t[..., None, :]
        decay_factor = jnp.where(causal, jnp.exp(jnp.where(causal, decay_gap, 0.0)), 0.0)
        weights = (scores[:, :, None] * decay_factor * step_t[..., None, :]).astype(jnp.bfloat16)
        within = jnp.einsum('sgetu,sugep->stgep', weights.astype(jnp.float32), heads_x)
        entering = lax.optimization_barrier(state_now.astype(jnp.bfloat16))
        carried_out = jnp.einsum('stgn,sgepn->stgep', group_c, entering.astype(jnp.float32))
        carried_out = carried_out * jnp.exp(cumulative_decay)[..., None]
        block_end = cum_t[..., -1]
        end_weight = jnp.exp(block_end[..., None] - cum_t) * step_t
        scaled_x = lax.optimization_barrier((heads_x * end_weight.transpose(0, 3, 1, 2)[..., None]).astype(jnp.bfloat16))
        block_state = jnp.einsum('sugep,sugn->sgepn', scaled_x.astype(jnp.float32), group_b)
        next_state = state_now * jnp.exp(block_end)[..., None, None] + block_state
        mixed_ssd = (within + carried_out).reshape(seq_count, BLOCK, INNER) * jax.nn.silu(output_gate_rows.astype(jnp.float32))
        grouped = mixed_ssd.reshape(seq_count, BLOCK, GROUPS, INNER // GROUPS)
        normed = grouped * lax.rsqrt(lax.optimization_barrier(jnp.mean(grouped * grouped, axis=-1, keepdims=True)) + eps)
        ssd_out = (normed.reshape(seq_count, BLOCK, INNER) * group_norm_gain.astype(jnp.float32)).astype(jnp.bfloat16)
        positions = (current_block_index * BLOCK + jnp.arange(BLOCK, dtype=jnp.int32)).astype(jnp.float32)
        pool_out = pool_mix(pooling_rows, prior_pool, positions, group_ids, pooling_group_weight, pooling_channel_scale)
        flat_ssd = ssd_out.reshape(seq_count * BLOCK, INNER)
        flat_pool = pool_out.reshape(seq_count * BLOCK, POOL)
        total = jnp.zeros((seq_count * BLOCK, D), jnp.float32)
        for part_index in range(N_TP):
            partial_value = jnp.dot(flat_ssd[:, part_index * share_ssd:(part_index + 1) * share_ssd], statespace_output_weight[part_index * share_ssd:(part_index + 1) * share_ssd], preferred_element_type=jnp.float32)
            partial_value = partial_value + jnp.dot(flat_pool[:, part_index * share_pool:(part_index + 1) * share_pool], pooling_output_weight[part_index * share_pool:(part_index + 1) * share_pool], preferred_element_type=jnp.float32)
            rounded = lax.optimization_barrier(partial_value.astype(jnp.bfloat16))
            total = total + rounded.astype(jnp.float32)
        inv_root = lax.rsqrt(lax.optimization_barrier(jnp.mean(total * total, axis=1, keepdims=True)) + eps)
        output = (total * inv_root * output_norm_gain.astype(jnp.float32)).astype(jnp.bfloat16)
        next_carry = (next_state, head_channel_rows[:, BLOCK - CONV + 1:], input_projection_rows[:, BLOCK - CONV + 1:], output_projection_rows[:, BLOCK - CONV + 1:], pooling_rows[:, BLOCK - pool_tail:])
        return (next_carry, output.reshape(seq_count, BLOCK, D))
    start_carry = (jnp.zeros((seq_count, GROUPS, per_group, HEAD_DIM, STATE), jnp.float32), jnp.zeros((seq_count, CONV - 1, INNER), jnp.bfloat16), jnp.zeros((seq_count, CONV - 1, GROUPS * STATE), jnp.bfloat16), jnp.zeros((seq_count, CONV - 1, GROUPS * STATE), jnp.bfloat16), jnp.zeros((seq_count, pool_tail, POOL), jnp.bfloat16))
    final_carry, outputs = lax.scan(advance, start_carry, mixer_inputs)
    return jnp.moveaxis(outputs, 0, 1).reshape(seq_count, SEQUENCE_TOKENS, D)
```

```python
import functools

import jax
import jax.numpy as jnp
from jax import lax
from jax.experimental import pallas as pl
from jax.experimental.pallas import tpu as pltpu
from jax.sharding import PartitionSpec as P

D = 4096
HEAD_DIM = 64
STATE = 128
CONV = 4
BLOCK = 128
POOL_GROUPS = 4
POOL_GROUP = 256


eps = 1e-06


def passed_along(block, axis, distance):
    devices = range(lax.axis_size(axis))
    route = [(i - distance, i) for i in devices if i - distance in devices]
    return lax.ppermute(block, axis, route)


def entering_2(array, axis, join, neutral):
    place = lax.axis_index(axis)
    gathered = jax.tree.map(
        lambda a, kind: lax.all_gather(a.astype(kind), axis), array, (jnp.bfloat16, jnp.bfloat16)
    )
    state = jax.tree.map(lambda a, e: jnp.zeros_like(a) + jnp.asarray(e, a.dtype), array, neutral)

    def one(lap, state):
        return join(
            state,
            jax.tree.map(
                lambda a, own: lax.dynamic_index_in_dim(a, lap, 0, False).astype(own.dtype),
                gathered,
                array,
            ),
        )

    return lax.fori_loop(0, place, one, state)


MESH_IDS = pl.DeviceIdType.MESH


def ring_place(index, size):
    if size != 4:
        return index
    return index + (index // 2) * (1 - 2 * (index % 2))


class Ring:
    def __init__(self, axis, size, folded):
        self.axis, self.size, self.folded = axis, size, folded
        me = lax.axis_index(axis)
        self.place = ring_place(me, size) if folded else me

    def at(self, offset):
        spot = lax.rem(self.place + offset + 2 * self.size, self.size)
        return ring_place(spot, self.size) if self.folded else spot

    def hops(self):
        found = []
        for step in range(1, self.size // 2 + 1):
            halved = self.size % 2 == 0 and step == self.size // 2
            found.append((step, 1, halved))
            found.append((step, -1, halved))
        return found

    def offsets(self):
        found = [0]
        for step, way, halved in self.hops():
            if not (halved and way == -1):
                found.append(-way * step)
        return found


class Gather:
    def __init__(self, own, whole, sends, arrivals, sp_size, fs_size):
        self.own, self.whole = own, whole
        self.sends, self.arrivals = sends, arrivals
        self.count = 0
        self.width = own.shape[1]
        self.fs_size = fs_size
        self.sp = Ring("sp", sp_size, False)
        self.fs = Ring("fs", fs_size, True)
        self.live = {}

    def columns(self, sp_off, fs_off):
        at = (self.sp.at(sp_off) * self.fs_size + self.fs.at(fs_off)) * self.width
        return pl.ds(pl.multiple_of(at, self.width), self.width)

    def start(self, key, ring, way, rows, sp_off, fs_off):
        first = sp_off == 0 and fs_off == 0
        cols = self.columns(sp_off, fs_off)
        src = self.own.at[rows] if first else self.whole.at[rows, cols]
        copy = pltpu.make_async_remote_copy(
            src_ref=src,
            dst_ref=self.whole.at[rows, cols],
            send_sem=self.sends.at[self.count],
            recv_sem=self.arrivals.at[self.count],
            device_id={ring.axis: ring.at(way)},
            device_id_type=MESH_IDS,
        )
        copy.start()
        self.count += 1
        self.live[key] = copy

    def barrier(self):
        barrier = pltpu.get_barrier_semaphore()
        total = 0
        for ring in (self.sp, self.fs):
            if ring.size > 1:
                for way in (1, -1):
                    pl.semaphore_signal(
                        barrier, inc=1, device_id={ring.axis: ring.at(way)}, device_id_type=MESH_IDS
                    )
                    total += 1
        if total:
            pl.semaphore_wait(barrier, total)

    def send(self, part, stage, cross, step, way, halved):
        rows_all = self.own.shape[0]
        low, high = (0, rows_all // 2) if part == 0 else (rows_all // 2, rows_all)
        ring = (self.fs, self.sp)[(part + stage) % 2]
        if halved:
            mid = low + (high - low) // 2
            low, high = (low, mid) if way == 1 else (mid, high)
        off = -way * (step - 1)
        sp_off, fs_off = (off, cross) if ring is self.sp else (cross, off)
        self.start((part, stage, cross, step, way), ring, way, pl.ds(low, high - low), sp_off, fs_off)

    def run(self):
        first = [(self.fs, self.sp)[part] for part in (0, 1)]
        then = [(self.sp, self.fs)[part] for part in (0, 1)]

        def send_at(stage, part, cross, step):
            ring = (first, then)[stage][part]
            for s, way, halved in ring.hops():
                if s == step:
                    self.send(part, stage, cross, s, way, halved)

        def wait_at(stage, part, cross, step):
            ring = (first, then)[stage][part]
            for s, way, halved in ring.hops():
                if s == step:
                    self.live[(part, stage, cross, s, way)].wait_recv()

        last = max(self.sp.size, self.fs.size) // 2
        for part in (0, 1):
            send_at(0, part, 0, 1)
        for part in (0, 1):
            send_at(1, part, 0, 1)
        for step in range(1, last + 1):
            for part in (0, 1):
                wait_at(0, part, 0, step)
                send_at(0, part, 0, step + 1)
            for part in (0, 1):
                for off in first[part].offsets():
                    if off and abs(off) == step:
                        send_at(1, part, off, 1)
        for step in range(1, last + 1):
            deepest = max(len(ring.offsets()) for ring in first)
            for spot in range(deepest):
                for part in (0, 1):
                    offsets = first[part].offsets()
                    if spot < len(offsets):
                        wait_at(1, part, offsets[spot], step)
                        send_at(1, part, offsets[spot], step + 1)

    def finish(self):
        for copy in self.live.values():
            copy.wait_send()


def hop_count(sp_size, fs_size):
    def hops(size):
        return 2 * (size // 2)

    return hops(sp_size) * (1 + fs_size) + hops(fs_size) * (1 + sp_size)


def gather_kernel(sp_size, fs_size, own, whole, sends, arrivals, local_sem):
    gather = Gather(own, whole, sends, arrivals, sp_size, fs_size)
    gather.barrier()
    mine = pltpu.make_async_copy(own, whole.at[:, gather.columns(0, 0)], local_sem)
    mine.start()
    gather.run()
    mine.wait()
    gather.finish()


def gathered_columns(own):
    sp_size, fs_size = lax.axis_size("sp"), lax.axis_size("fs")
    rows, width = own.shape
    if width % 128 or rows % 64:
        return lax.all_gather(own, ("sp", "fs"), axis=1, tiled=True)
    hops = hop_count(sp_size, fs_size)
    return pl.pallas_call(
        functools.partial(gather_kernel, sp_size, fs_size),
        out_shape=jax.ShapeDtypeStruct((rows, width * sp_size * fs_size), own.dtype),
        in_specs=[pl.BlockSpec(memory_space=pltpu.VMEM)],
        out_specs=pl.BlockSpec(memory_space=pltpu.VMEM),
        scratch_shapes=[
            pltpu.SemaphoreType.DMA((hops,)),
            pltpu.SemaphoreType.DMA((hops,)),
            pltpu.SemaphoreType.DMA,
        ],
        compiler_params=pltpu.CompilerParams(
            collective_id=0, has_side_effects=True, vmem_limit_bytes=40 * 2**20
        ),
        name="gather_columns",
    )(own)


def causal_taps(input_rows, prior_rows, tap_weights, offset_bias):
    padded = jnp.concatenate([prior_rows, input_rows], axis=0).astype(jnp.float32)
    tok_rows = input_rows.shape[0]
    running = jnp.zeros(input_rows.shape, jnp.float32) + offset_bias
    for tap_index in range(tap_weights.shape[0]):
        running = (
            running
            + tap_weights[tap_index].astype(jnp.float32) * padded[tap_index : tap_index + tok_rows]
        )
    return jax.nn.silu(running).astype(jnp.bfloat16)


def pool_mix(input_rows, prior_rows, positions, group_ids, local_weight, local_scale):
    tail_rows = prior_rows.shape[0]
    tok_rows = input_rows.shape[0]
    padded = jnp.concatenate([prior_rows, input_rows], axis=0).astype(jnp.float32)
    window_reach = jnp.left_shift(jnp.int32(2), group_ids)
    running = jnp.zeros(input_rows.shape, jnp.float32)
    for offset_back in range(tail_rows + 1):
        start_row = tail_rows - offset_back
        running = running + padded[start_row : start_row + tok_rows] * (
            offset_back < window_reach
        ).astype(jnp.float32)
    window_count = jnp.minimum(positions[:, None] + 1.0, window_reach.astype(jnp.float32)[None, :])
    pooled = (running / window_count - input_rows.astype(jnp.float32)).astype(jnp.bfloat16)
    grouped = pooled.reshape(tok_rows, local_weight.shape[0], local_weight.shape[1])
    mixed = jnp.einsum("lgc,gcd->lgd", grouped, local_weight, preferred_element_type=jnp.float32)
    return (mixed.reshape(input_rows.shape) * local_scale.astype(jnp.float32)).astype(jnp.bfloat16)


def join_states(earlier, later_part):
    return (
        earlier[0] + later_part[0],
        earlier[1] * jnp.exp(later_part[0])[..., None, None] + later_part[1],
    )


def body(
    statespace_input,
    output_gate_input,
    state_input_projection,
    state_output_projection,
    step_size_input,
    added_log_decay,
    logarithm_rates,
    head_channel_taps,
    input_projection_taps,
    output_projection_taps,
    input_projection_bias,
    group_norm_gain,
    pooling_input,
    pooling_group_weight,
    pooling_channel_scale,
    statespace_output_weight,
    pooling_output_weight,
    output_norm_gain,
):
    core_index = lax.axis_index("tp")
    core_count = lax.axis_size("tp")
    seq_index = lax.axis_index("sp")
    head_channel_rows = statespace_input[0]
    output_gate_rows = output_gate_input[0]
    input_projection_rows = state_input_projection[0]
    output_projection_rows = state_output_projection[0]
    step_size_rows = step_size_input[0]
    decay_spikes = added_log_decay[0]
    pooling_rows = pooling_input[0]
    tok_rows = head_channel_rows.shape[0]
    inner_local = head_channel_rows.shape[1]
    heads_local = step_size_rows.shape[1]
    state_local = input_projection_rows.shape[1]
    pool_local = pooling_rows.shape[1]
    groups_local = state_local // STATE
    per_group = heads_local // groups_local
    groups_pool = pool_local // POOL_GROUP
    pool_tail = 2**POOL_GROUPS - 1
    conv_tail = CONV - 1
    own_columns = jnp.concatenate([statespace_output_weight, pooling_output_weight], axis=0)
    whole_columns = gathered_columns(own_columns)
    tails = jnp.concatenate(
        [
            jnp.pad(rows[tok_rows - tail :], ((pool_tail - tail, 0), (0, 0)))
            for rows, tail in (
                (head_channel_rows, conv_tail),
                (input_projection_rows, conv_tail),
                (output_projection_rows, conv_tail),
                (pooling_rows, pool_tail),
            )
        ],
        axis=1,
    )
    prior = passed_along(tails, "sp", 1)
    widths = (inner_local, state_local, state_local, pool_local)
    prior_x, prior_b, prior_c, prior_pool = (
        prior[pool_tail - tail :, sum(widths[:at]) : sum(widths[: at + 1])]
        for at, tail in enumerate((conv_tail, conv_tail, conv_tail, pool_tail))
    )
    taps_x = lax.dynamic_slice_in_dim(head_channel_taps, core_index * inner_local, inner_local, 1)
    taps_b = lax.dynamic_slice_in_dim(
        input_projection_taps, core_index * state_local, state_local, 1
    )
    taps_c = lax.dynamic_slice_in_dim(
        output_projection_taps, core_index * state_local, state_local, 1
    )
    bias_b = lax.dynamic_slice_in_dim(
        input_projection_bias, core_index * state_local, state_local, 0
    )
    gain_ssd = lax.dynamic_slice_in_dim(group_norm_gain, core_index * inner_local, inner_local, 0)
    head_decay_rates = jnp.exp(
        lax.dynamic_slice_in_dim(logarithm_rates, core_index * heads_local, heads_local, 0)
    )
    gain_pool = lax.dynamic_slice_in_dim(
        pooling_channel_scale, core_index * pool_local, pool_local, 0
    )
    weight_pool = lax.dynamic_slice_in_dim(
        pooling_group_weight, core_index * groups_pool, groups_pool, 0
    )
    x_conv = causal_taps(head_channel_rows, prior_x, taps_x, 0.0)
    b_conv = causal_taps(input_projection_rows, prior_b, taps_b, bias_b.astype(jnp.float32))
    c_conv = causal_taps(output_projection_rows, prior_c, taps_c, 0.0)
    blocks = tok_rows // BLOCK
    discrete_step_size = jax.nn.softplus(step_size_rows.astype(jnp.float32))
    logarithm_decay = -discrete_step_size * head_decay_rates + decay_spikes
    cumulative_decay = jnp.cumsum(
        logarithm_decay.reshape(blocks, BLOCK, groups_local, per_group), axis=1
    )
    cum_t = cumulative_decay.transpose(0, 2, 3, 1)
    step_t = discrete_step_size.reshape(blocks, BLOCK, groups_local, per_group).transpose(
        0, 2, 3, 1
    )
    heads_x = x_conv.reshape(blocks, BLOCK, groups_local, per_group, HEAD_DIM)
    group_b = b_conv.reshape(blocks, BLOCK, groups_local, STATE)
    group_c = c_conv.reshape(blocks, BLOCK, groups_local, STATE)
    scores = jnp.einsum("ktgn,kugn->kgtu", group_c, group_b, preferred_element_type=jnp.float32)
    causal = jnp.arange(BLOCK)[:, None] >= jnp.arange(BLOCK)[None, :]
    decay_gap = cum_t[..., :, None] - cum_t[..., None, :]
    decay_factor = jnp.where(causal, jnp.exp(jnp.where(causal, decay_gap, 0.0)), 0.0)
    weights = (scores[:, :, None] * decay_factor * step_t[..., None, :]).astype(jnp.bfloat16)
    within = jnp.einsum("kgetu,kugep->ktgep", weights, heads_x, preferred_element_type=jnp.float32)
    block_end = cum_t[..., -1]
    end_weight = jnp.exp(block_end[..., None] - cum_t) * step_t
    scaled_x = (heads_x * end_weight.transpose(0, 3, 1, 2)[..., None]).astype(jnp.bfloat16)
    block_state = jnp.einsum(
        "kugep,kugn->kgepn", scaled_x, group_b, preferred_element_type=jnp.float32
    )

    def local_chain(state_now, current_inputs):
        piece_state, piece_fall = current_inputs
        return (state_now * jnp.exp(piece_fall)[..., None, None] + piece_state, state_now)

    final_state, local_entering = lax.scan(
        local_chain, jnp.zeros(block_state.shape[1:], jnp.float32), (block_state, block_end)
    )
    log_total = jnp.sum(block_end, axis=0)
    prefix_log = jnp.cumsum(block_end, axis=0) - block_end
    log_before, state_before = entering_2(
        (log_total, final_state),
        "sp",
        join_states,
        (jnp.zeros_like(log_total), jnp.zeros_like(final_state)),
    )
    entering = (local_entering + jnp.exp(prefix_log)[..., None, None] * state_before[None]).astype(
        jnp.bfloat16
    )
    carried_out = jnp.einsum(
        "ktgn,kgepn->ktgep", group_c, entering, preferred_element_type=jnp.float32
    )
    carried_out = carried_out * jnp.exp(cumulative_decay)[..., None]
    mixed_ssd = (within + carried_out).reshape(tok_rows, inner_local) * jax.nn.silu(
        output_gate_rows.astype(jnp.float32)
    )
    grouped = mixed_ssd.reshape(tok_rows, groups_local, inner_local // groups_local)
    normed = grouped * lax.rsqrt(jnp.mean(grouped * grouped, axis=-1, keepdims=True) + eps)
    ssd_out = (normed.reshape(tok_rows, inner_local) * gain_ssd.astype(jnp.float32)).astype(
        jnp.bfloat16
    )
    positions = (seq_index * tok_rows + jnp.arange(tok_rows, dtype=jnp.int32)).astype(jnp.float32)
    group_ids = core_index * groups_pool + jnp.arange(pool_local, dtype=jnp.int32) // POOL_GROUP
    pool_out = pool_mix(pooling_rows, prior_pool, positions, group_ids, weight_pool, gain_pool)
    half_width = D // core_count
    gain_out = lax.dynamic_slice_in_dim(
        output_norm_gain, core_index * half_width, half_width, 0
    ).astype(jnp.float32)
    channels = jnp.concatenate([ssd_out, pool_out], axis=1)
    partial = jnp.dot(channels, whole_columns, preferred_element_type=jnp.float32).astype(
        jnp.bfloat16
    )
    own_half = lax.dynamic_slice_in_dim(partial, core_index * half_width, half_width, 1).astype(
        jnp.float32
    )
    for hop in range(1, core_count):
        target = lax.rem(core_index + hop, core_count)
        leaving = lax.dynamic_slice_in_dim(partial, target * half_width, half_width, 1)
        route = [(i, (i + hop) % core_count) for i in range(core_count)]
        own_half = own_half + lax.ppermute(leaving, "tp", route).astype(jnp.float32)
    row_squares = lax.psum(jnp.sum(own_half * own_half, axis=1), "tp")
    result = own_half * lax.rsqrt(row_squares / D + eps)[:, None] * gain_out
    return result.astype(jnp.bfloat16)[None]


def solution(mesh):
    in_specs = (
        P("fs", "sp", "tp"),
        P("fs", "sp", "tp"),
        P("fs", "sp", "tp"),
        P("fs", "sp", "tp"),
        P("fs", "sp", "tp"),
        P("fs", "sp", "tp"),
        P(),
        P(),
        P(),
        P(),
        P(),
        P(),
        P("fs", "sp", "tp"),
        P(),
        P(),
        P("tp", ("sp", "fs")),
        P("tp", ("sp", "fs")),
        P(),
    )
    out_specs = P("fs", "sp", "tp")
    return jax.shard_map(body, mesh=mesh, in_specs=in_specs, out_specs=out_specs, check_vma=False)
```

```python
import functools

import jax
import jax.numpy as jnp
from jax import lax
from jax.experimental import pallas as pl
from jax.experimental.pallas import tpu as pltpu
from jax.sharding import PartitionSpec as P

D = 4096
HEAD_DIM = 64
STATE = 128
CONV = 4
BLOCK = 128
POOL_GROUPS = 4
POOL_GROUP = 256


eps = 1e-06


def passed_along(block, axis, distance):
    devices = range(lax.axis_size(axis))
    route = [(i - distance, i) for i in devices if i - distance in devices]
    return lax.ppermute(block, axis, route)


def entering_2(array, axis, join, neutral):
    place = lax.axis_index(axis)
    gathered = jax.tree.map(
        lambda a, kind: lax.all_gather(a.astype(kind), axis), array, (jnp.bfloat16, jnp.bfloat16)
    )
    state = jax.tree.map(lambda a, e: jnp.zeros_like(a) + jnp.asarray(e, a.dtype), array, neutral)

    def one(lap, state):
        return join(
            state,
            jax.tree.map(
                lambda a, own: lax.dynamic_index_in_dim(a, lap, 0, False).astype(own.dtype),
                gathered,
                array,
            ),
        )

    return lax.fori_loop(0, place, one, state)


MESH_IDS = pl.DeviceIdType.MESH
EXACT = lax.Precision.HIGHEST


def ring_place(index, size):
    if size != 4:
        return index
    return index + (index // 2) * (1 - 2 * (index % 2))


class Gather:
    def __init__(self, own, whole, sends, arrivals, sp_size, fs_size):
        self.own, self.whole = own, whole
        self.sends, self.arrivals = sends, arrivals
        self.width = own.shape[1]
        self.sp_size, self.fs_size = sp_size, fs_size
        self.sp_me = lax.axis_index("sp")
        self.fs_me = ring_place(lax.axis_index("fs"), fs_size)
        rows = own.shape[0]
        self.cut = rows * 3 // 4 // 64 * 64
        self.keys = {}
        self.fs_last = fs_size // 2
        self.fs_offsets = [0]
        for step in range(1, self.fs_last + 1):
            self.fs_offsets.append(-step)
            if not self.halved(step):
                self.fs_offsets.append(step)

    def halved(self, step):
        return self.fs_size % 2 == 0 and step == self.fs_last

    def fs_at(self, offset):
        return ring_place(lax.rem(self.fs_me + offset + 2 * self.fs_size, self.fs_size), self.fs_size)

    def copy(self, part, stage, cross, step, way):
        on_sp = part == stage
        low, high = (0, self.cut) if part == 0 else (self.cut, self.own.shape[0])
        if not on_sp and self.halved(step):
            mid = low + (high - low) // 2
            low, high = (low, mid) if way == 1 else (mid, high)
        rows = pl.ds(low, high - low)
        off = -way * (step - 1)
        sp_off, fs_off = (off, cross) if on_sp else (cross, off)
        at = ((self.sp_me + sp_off) * self.fs_size + self.fs_at(fs_off)) * self.width
        cols = pl.ds(pl.multiple_of(at, self.width), self.width)
        first = sp_off == 0 and fs_off == 0
        spot = self.keys.setdefault((part, stage, cross, step, way), len(self.keys))
        return pltpu.make_async_remote_copy(
            src_ref=self.own.at[rows] if first else self.whole.at[rows, cols],
            dst_ref=self.whole.at[rows, cols],
            send_sem=self.sends.at[spot],
            recv_sem=self.arrivals.at[spot],
            device_id={"sp": self.sp_me + way} if on_sp else {"fs": self.fs_at(way)},
            device_id_type=MESH_IDS,
        )

    def when(self, part, stage, cross, step, way, arriving):
        if part == stage:
            gone = step if arriving else step - 1
            origin = self.sp_me - way * gone
            far = self.sp_me if arriving else self.sp_me + way
            checks = [origin >= 0, origin < self.sp_size, far >= 0, far < self.sp_size]
        elif cross:
            checks = [self.sp_me + cross >= 0, self.sp_me + cross < self.sp_size]
        else:
            return None
        return functools.reduce(jnp.logical_and, checks)

    def each(self, part, stage, cross, step, arriving, act):
        last = self.sp_size - 1 if part == stage else self.fs_last
        if not 1 <= step <= last:
            return
        for way in (1, -1):
            key = (part, stage, cross, step, way)
            here = self.when(*key, arriving)

            def run(key=key):
                act(self.copy(*key))

            if here is None:
                run()
            else:
                pl.when(here)(run)

    def send(self, *key):
        self.each(*key, False, lambda copy: copy.start())

    def take(self, *key):
        self.each(*key, True, lambda copy: copy.wait_recv())

    def barrier(self):
        barrier = pltpu.get_barrier_semaphore()
        total = 0
        for far in range(1, self.sp_size):
            other = lax.rem(self.sp_me + far, self.sp_size)
            pl.semaphore_signal(barrier, inc=1, device_id={"sp": other}, device_id_type=MESH_IDS)
            total += 1
        if self.fs_size > 1:
            for way in (1, -1):
                other = self.fs_at(way)
                pl.semaphore_signal(
                    barrier, inc=1, device_id={"fs": other}, device_id_type=MESH_IDS
                )
                total += 1
        if total:
            pl.semaphore_wait(barrier, total)

    def pair(self, off):
        return [0] if off == 0 else [-off, off]

    def run(self):
        rounds = max(self.sp_size - 1, self.fs_last)
        self.send(0, 0, 0, 1)
        self.send(1, 0, 0, 1)
        self.send(0, 1, 0, 1)
        for step in range(1, rounds + 1):
            yield
            self.take(0, 0, 0, step)
            self.send(0, 0, 0, step + 1)
            if step < self.sp_size:
                for cross in self.pair(step):
                    self.send(0, 1, cross, 1)
            if step == 1:
                self.send(1, 1, 0, 1)
            self.take(1, 0, 0, step)
            self.send(1, 0, 0, step + 1)
            for cross in self.fs_offsets[1:]:
                if abs(cross) == step:
                    self.send(1, 1, cross, 1)
            yield
            if step <= self.sp_size:
                for cross in self.pair(step - 1):
                    self.take(0, 1, cross, 1)
                    self.send(0, 1, cross, 2)
            yield
            if step > self.fs_last:
                for cross in self.fs_offsets:
                    self.take(1, 1, cross, step - self.fs_last)
                    self.send(1, 1, cross, step - self.fs_last + 1)
        for late in range(rounds, self.sp_size):
            yield
            for cross in self.pair(late):
                self.take(0, 1, cross, 1)
                self.send(0, 1, cross, 2)
        for step in range(max(rounds - self.fs_last, 0) + 1, self.sp_size):
            for cross in self.fs_offsets:
                yield
                self.take(1, 1, cross, step)
                self.send(1, 1, cross, step + 1)
        for step in range(2, self.fs_last + 1):
            for off in range(self.sp_size):
                yield
                for cross in self.pair(off):
                    self.take(0, 1, cross, step)
                    self.send(0, 1, cross, step + 1)

    def finish(self):
        for key in list(self.keys):
            part, stage, cross, step, way = key
            here = self.when(*key, False)

            def run(key=key):
                self.copy(*key).wait_send()

            if here is None:
                run()
            else:
                pl.when(here)(run)


def hop_count(sp_size, fs_size):
    along, around = 2 * (sp_size - 1), 2 * (fs_size // 2)
    return along * (1 + fs_size) + around * (1 + 2 * sp_size - 1)


def silu(rows):
    return rows / (1.0 + jnp.exp(-rows))


def softplus(rows):
    return jnp.maximum(rows, 0.0) + jnp.log(1.0 + jnp.exp(-jnp.abs(rows)))


def mixers(sizes, refs, links):
    sp_size, tail = sizes
    (x_in, gate, bc_in, dt, dt_t, added, added_t, rates, rates_t, x_taps, bc_taps, bc_bias, gain,
     pool_in, pool_weight, pool_scale, reach, prior, channels, x_pad, bc_pad, pool_pad, x_conv,
     bc_conv, within, grown, local_in, state, ends, before, far_state, far_log) = refs
    sends, arrivals = links
    rows, inner = x_in.shape
    heads = dt.shape[1]
    wide = bc_in.shape[1] // 2
    groups = wide // STATE
    span = inner // groups
    blocks = rows // BLOCK
    sp_me = lax.axis_index("sp")
    x_pad[0:tail] = prior[:, 0:inner].astype(jnp.float32)
    bc_pad[0:tail] = prior[:, inner : inner + 2 * wide].astype(jnp.float32)
    pool_pad[0:tail] = prior[:, inner + 2 * wide :].astype(jnp.float32)
    x_pad[tail:] = x_in[...].astype(jnp.float32)
    bc_pad[tail:] = bc_in[...].astype(jnp.float32)
    pool_pad[tail:] = pool_in[...].astype(jnp.float32)
    step_all = softplus(dt[...].astype(jnp.float32))
    log_all = -step_all * jnp.exp(rates[...]) + added[...]
    step_flat = softplus(dt_t[...].astype(jnp.float32))
    log_flat = -step_flat * jnp.exp(rates_t[...]) + added_t[...]
    down = lax.broadcasted_iota(jnp.int32, (BLOCK, BLOCK), 0)
    across = lax.broadcasted_iota(jnp.int32, (BLOCK, BLOCK), 1)
    causal = down >= across
    lower = causal.astype(jnp.float32)
    upper = (down <= across).astype(jnp.float32)
    first_half = lax.broadcasted_iota(jnp.int32, (BLOCK, 2 * HEAD_DIM), 1) < HEAD_DIM
    yield

    def taps(pad, weights, at, cols):
        total = None
        for tap in range(CONV):
            begin = at * BLOCK + tail - CONV + 1 + tap
            term = pad[begin : begin + BLOCK, cols] * weights[tap : tap + 1, cols].astype(
                jnp.float32
            )
            total = term if total is None else total + term
        return total

    state[...] = jnp.zeros_like(state)
    for at in range(blocks):
        now = slice(at * BLOCK, (at + 1) * BLOCK)
        every = slice(0, 2 * wide)
        bc_conv[now] = silu(
            taps(bc_pad, bc_taps, at, every) + bc_bias[...].astype(jnp.float32)
        ).astype(jnp.bfloat16)
        cum = jnp.dot(lower, log_all[now], precision=EXACT, preferred_element_type=jnp.float32)
        cum_flat = jnp.dot(
            log_flat[:, now], upper, precision=EXACT, preferred_element_type=jnp.float32
        )
        step_row = step_flat[:, now]
        for group in range(groups):
            cols = slice(group * span, (group + 1) * span)
            x_now = silu(taps(x_pad, x_taps, at, cols))
            x_half = x_now.astype(jnp.bfloat16)
            b_now = bc_conv[now, group * STATE : (group + 1) * STATE]
            c_now = bc_conv[now, wide + group * STATE : wide + (group + 1) * STATE]
            spread = (
                lax.broadcasted_iota(jnp.int32, (heads, span), 0)
                == group * (span // HEAD_DIM)
                + lax.broadcasted_iota(jnp.int32, (heads, span), 1) // HEAD_DIM
            ).astype(jnp.float32)
            cum_wide = jnp.dot(cum, spread, precision=EXACT, preferred_element_type=jnp.float32)
            step_wide = jnp.dot(
                step_all[now], spread, precision=EXACT, preferred_element_type=jnp.float32
            )
            grown[now, cols] = jnp.exp(cum_wide)
            end = cum_wide[BLOCK - 1 : BLOCK]
            ends[at : at + 1, cols] = end
            scaled = (x_half.astype(jnp.float32) * jnp.exp(end - cum_wide) * step_wide).astype(
                jnp.bfloat16
            )
            b_flat = jnp.transpose(b_now.astype(jnp.float32)).astype(jnp.bfloat16)
            local_in[at, :, cols] = state[:, cols]
            state[:, cols] = state[:, cols] * jnp.exp(end) + jnp.dot(
                b_flat, scaled, preferred_element_type=jnp.float32
            )
            scores = jnp.dot(c_now, b_flat, preferred_element_type=jnp.float32)
            for pair in range(span // (2 * HEAD_DIM)):
                lanes = slice(pair * 2 * HEAD_DIM, (pair + 1) * 2 * HEAD_DIM)
                both = []
                for side in range(2):
                    head = group * (span // HEAD_DIM) + 2 * pair + side
                    gap = cum[:, head : head + 1] - cum_flat[head : head + 1]
                    decay = jnp.exp(jnp.where(causal, gap, -1e30))
                    weights = (scores * decay * step_row[head : head + 1]).astype(jnp.bfloat16)
                    both.append(
                        jnp.dot(weights, x_half[:, lanes], preferred_element_type=jnp.float32)
                    )
                here = group * span + pair * 2 * HEAD_DIM
                within[now, here : here + 2 * HEAD_DIM] = jnp.where(first_half, both[0], both[1])
            yield
    total_log = ends[0:1]
    for at in range(1, blocks):
        total_log = total_log + ends[at : at + 1]
    far_state[sp_size] = state[...].astype(jnp.bfloat16)
    far_log[sp_size] = jnp.broadcast_to(total_log, far_log.shape[1:])

    def letters(far):
        return [
            pltpu.make_async_remote_copy(
                src_ref=buffer.at[sp_size],
                dst_ref=buffer.at[far - 1],
                send_sem=sends.at[far - 1, kind],
                recv_sem=arrivals.at[far - 1, kind],
                device_id={"sp": sp_me + far},
                device_id_type=MESH_IDS,
            )
            for kind, buffer in enumerate((far_state, far_log))
        ]

    for far in range(1, sp_size):

        @pl.when(sp_me + far < sp_size)
        def _(far=far):
            for letter in letters(far):
                letter.start()

    yield
    place = sp_me * rows
    for group in range(pool_weight.shape[0]):
        cols = slice(group * POOL_GROUP, (group + 1) * POOL_GROUP)
        window = reach[:, cols]
        for at in range(blocks):
            now = slice(at * BLOCK, (at + 1) * BLOCK)
            running = None
            for back in range(tail):
                begin = at * BLOCK + tail - back
                term = pool_pad[begin : begin + BLOCK, cols] * jnp.where(back < window, 1.0, 0.0)
                running = term if running is None else running + term
            position = (
                place + at * BLOCK + lax.broadcasted_iota(jnp.int32, (BLOCK, POOL_GROUP), 0)
            ).astype(jnp.float32)
            pooled = running / jnp.minimum(position + 1.0, window) - pool_in[now, cols].astype(
                jnp.float32
            )
            mixed = jnp.dot(
                pooled.astype(jnp.bfloat16), pool_weight[group], preferred_element_type=jnp.float32
            )
            out = inner + group * POOL_GROUP
            channels[now, out : out + POOL_GROUP] = (
                mixed * pool_scale[:, cols].astype(jnp.float32)
            ).astype(jnp.bfloat16)
        yield
    before[...] = jnp.zeros_like(before)
    for far in range(sp_size - 1, 0, -1):

        @pl.when(sp_me - far >= 0)
        def _(far=far):
            for letter in letters(far):
                letter.wait_recv()
            before[...] = before[...] * jnp.exp(far_log[far - 1][0:1]) + far_state[far - 1].astype(
                jnp.float32
            )

    yield
    prefix = jnp.zeros_like(total_log)
    for at in range(blocks):
        now = slice(at * BLOCK, (at + 1) * BLOCK)
        for group in range(groups):
            cols = slice(group * span, (group + 1) * span)
            entering = local_in[at, :, cols] + jnp.exp(prefix[:, cols]) * before[:, cols]
            c_now = bc_conv[now, wide + group * STATE : wide + (group + 1) * STATE]
            carried = jnp.dot(
                c_now, entering.astype(jnp.bfloat16), preferred_element_type=jnp.float32
            )
            mixed = (within[now, cols] + carried * grown[now, cols]) * silu(
                gate[now, cols].astype(jnp.float32)
            )
            root = lax.rsqrt(jnp.mean(mixed * mixed, axis=1, keepdims=True) + eps)
            channels[now, cols] = (mixed * root * gain[:, cols].astype(jnp.float32)).astype(
                jnp.bfloat16
            )
        prefix = prefix + ends[at : at + 1]
        yield
    for far in range(1, sp_size):

        @pl.when(sp_me + far < sp_size)
        def _(far=far):
            for letter in letters(far):
                letter.wait_send()


def whole_kernel(sp_size, fs_size, tail, own, *refs):
    inputs, (whole, channels), scratch = refs[:18], refs[18:20], refs[20:]
    sends, arrivals, local_sem, letter_sends, letter_arrivals = scratch[:5]
    gather = Gather(own, whole, sends, arrivals, sp_size, fs_size)
    gather.barrier()
    at = (gather.sp_me * fs_size + gather.fs_at(0)) * gather.width
    mine = pltpu.make_async_copy(
        own, whole.at[:, pl.ds(pl.multiple_of(at, gather.width), gather.width)], local_sem
    )
    mine.start()
    moves = gather.run()
    work = mixers(
        (sp_size, tail), (*inputs, channels, *scratch[5:]), (letter_sends, letter_arrivals)
    )
    next(moves, None)
    for _ in work:
        next(moves, None)
    for _ in moves:
        pass
    mine.wait()
    gather.finish()


def mixed_and_gathered(own, inputs, tail):
    sp_size, fs_size = lax.axis_size("sp"), lax.axis_size("fs")
    rows, width = own.shape
    x_in, bc_in, pool_in = inputs[0], inputs[2], inputs[13]
    tok_rows, inner = x_in.shape
    blocks = tok_rows // BLOCK
    hops = hop_count(sp_size, fs_size)
    vmem = pl.BlockSpec(memory_space=pltpu.VMEM)
    return pl.pallas_call(
        functools.partial(whole_kernel, sp_size, fs_size, tail),
        out_shape=(
            jax.ShapeDtypeStruct((rows, width * sp_size * fs_size), own.dtype),
            jax.ShapeDtypeStruct((tok_rows, inner + pool_in.shape[1]), jnp.bfloat16),
        ),
        in_specs=[vmem] * (1 + len(inputs)),
        out_specs=(vmem, vmem),
        scratch_shapes=[
            pltpu.SemaphoreType.DMA((hops,)),
            pltpu.SemaphoreType.DMA((hops,)),
            pltpu.SemaphoreType.DMA,
            pltpu.SemaphoreType.DMA((sp_size, 2)),
            pltpu.SemaphoreType.DMA((sp_size, 2)),
            pltpu.VMEM((tail + tok_rows, inner), jnp.float32),
            pltpu.VMEM((tail + tok_rows, bc_in.shape[1]), jnp.float32),
            pltpu.VMEM((tail + tok_rows, pool_in.shape[1]), jnp.float32),
            pltpu.VMEM((8, 128), jnp.bfloat16),
            pltpu.VMEM((tok_rows, bc_in.shape[1]), jnp.bfloat16),
            pltpu.VMEM((tok_rows, inner), jnp.float32),
            pltpu.VMEM((tok_rows, inner), jnp.float32),
            pltpu.VMEM((blocks, STATE, inner), jnp.float32),
            pltpu.VMEM((STATE, inner), jnp.float32),
            pltpu.VMEM((-(-blocks // 8) * 8, inner), jnp.float32),
            pltpu.VMEM((STATE, inner), jnp.float32),
            pltpu.VMEM((sp_size + 1, STATE, inner), jnp.bfloat16),
            pltpu.VMEM((sp_size + 1, 8, inner), jnp.float32),
        ],
        compiler_params=pltpu.CompilerParams(
            collective_id=0, has_side_effects=True, vmem_limit_bytes=48 * 2**20
        ),
        name="mega_mixers",
    )(own, *inputs)


def causal_taps(input_rows, prior_rows, tap_weights, offset_bias):
    padded = jnp.concatenate([prior_rows, input_rows], axis=0).astype(jnp.float32)
    tok_rows = input_rows.shape[0]
    running = jnp.zeros(input_rows.shape, jnp.float32) + offset_bias
    for tap_index in range(tap_weights.shape[0]):
        running = (
            running
            + tap_weights[tap_index].astype(jnp.float32) * padded[tap_index : tap_index + tok_rows]
        )
    return jax.nn.silu(running).astype(jnp.bfloat16)


def pool_mix(input_rows, prior_rows, positions, group_ids, local_weight, local_scale):
    tail_rows = prior_rows.shape[0]
    tok_rows = input_rows.shape[0]
    padded = jnp.concatenate([prior_rows, input_rows], axis=0).astype(jnp.float32)
    window_reach = jnp.left_shift(jnp.int32(2), group_ids)
    running = jnp.zeros(input_rows.shape, jnp.float32)
    for offset_back in range(tail_rows + 1):
        start_row = tail_rows - offset_back
        running = running + padded[start_row : start_row + tok_rows] * (
            offset_back < window_reach
        ).astype(jnp.float32)
    window_count = jnp.minimum(positions[:, None] + 1.0, window_reach.astype(jnp.float32)[None, :])
    pooled = (running / window_count - input_rows.astype(jnp.float32)).astype(jnp.bfloat16)
    grouped = pooled.reshape(tok_rows, local_weight.shape[0], local_weight.shape[1])
    mixed = jnp.einsum("lgc,gcd->lgd", grouped, local_weight, preferred_element_type=jnp.float32)
    return (mixed.reshape(input_rows.shape) * local_scale.astype(jnp.float32)).astype(jnp.bfloat16)


def join_states(earlier, later_part):
    return (
        earlier[0] + later_part[0],
        earlier[1] * jnp.exp(later_part[0])[..., None, None] + later_part[1],
    )


def body(
    statespace_input,
    output_gate_input,
    state_input_projection,
    state_output_projection,
    step_size_input,
    added_log_decay,
    logarithm_rates,
    head_channel_taps,
    input_projection_taps,
    output_projection_taps,
    input_projection_bias,
    group_norm_gain,
    pooling_input,
    pooling_group_weight,
    pooling_channel_scale,
    statespace_output_weight,
    pooling_output_weight,
    output_norm_gain,
):
    core_index = lax.axis_index("tp")
    core_count = lax.axis_size("tp")
    seq_index = lax.axis_index("sp")
    head_channel_rows = statespace_input[0]
    output_gate_rows = output_gate_input[0]
    input_projection_rows = state_input_projection[0]
    output_projection_rows = state_output_projection[0]
    step_size_rows = step_size_input[0]
    decay_spikes = added_log_decay[0]
    pooling_rows = pooling_input[0]
    tok_rows = head_channel_rows.shape[0]
    inner_local = head_channel_rows.shape[1]
    heads_local = step_size_rows.shape[1]
    state_local = input_projection_rows.shape[1]
    pool_local = pooling_rows.shape[1]
    groups_local = state_local // STATE
    per_group = heads_local // groups_local
    groups_pool = pool_local // POOL_GROUP
    pool_tail = 2**POOL_GROUPS - 1
    conv_tail = CONV - 1
    own_columns = jnp.concatenate([statespace_output_weight, pooling_output_weight], axis=0)
    tails = jnp.concatenate(
        [
            jnp.pad(rows[tok_rows - tail :], ((pool_tail - tail, 0), (0, 0)))
            for rows, tail in (
                (head_channel_rows, conv_tail),
                (input_projection_rows, conv_tail),
                (output_projection_rows, conv_tail),
                (pooling_rows, pool_tail),
            )
        ],
        axis=1,
    )
    prior = passed_along(tails, "sp", 1)
    widths = (inner_local, state_local, state_local, pool_local)
    prior_x, prior_b, prior_c, prior_pool = (
        prior[pool_tail - tail :, sum(widths[:at]) : sum(widths[: at + 1])]
        for at, tail in enumerate((conv_tail, conv_tail, conv_tail, pool_tail))
    )
    taps_x = lax.dynamic_slice_in_dim(head_channel_taps, core_index * inner_local, inner_local, 1)
    taps_b = lax.dynamic_slice_in_dim(
        input_projection_taps, core_index * state_local, state_local, 1
    )
    taps_c = lax.dynamic_slice_in_dim(
        output_projection_taps, core_index * state_local, state_local, 1
    )
    bias_b = lax.dynamic_slice_in_dim(
        input_projection_bias, core_index * state_local, state_local, 0
    )
    gain_ssd = lax.dynamic_slice_in_dim(group_norm_gain, core_index * inner_local, inner_local, 0)
    head_decay_rates = jnp.exp(
        lax.dynamic_slice_in_dim(logarithm_rates, core_index * heads_local, heads_local, 0)
    )
    gain_pool = lax.dynamic_slice_in_dim(
        pooling_channel_scale, core_index * pool_local, pool_local, 0
    )
    weight_pool = lax.dynamic_slice_in_dim(
        pooling_group_weight, core_index * groups_pool, groups_pool, 0
    )
    tail = pool_tail + 1
    local_width = own_columns.shape[1]
    narrow = local_width % 128 != 0 or lax.axis_size("sp") > 8
    if narrow:
        whole_columns = lax.all_gather(own_columns, ("sp", "fs"), axis=1, tiled=True)
        x_conv = causal_taps(head_channel_rows, prior_x, taps_x, 0.0)
        b_conv = causal_taps(input_projection_rows, prior_b, taps_b, bias_b.astype(jnp.float32))
        c_conv = causal_taps(output_projection_rows, prior_c, taps_c, 0.0)
        blocks = tok_rows // BLOCK
        discrete_step_size = jax.nn.softplus(step_size_rows.astype(jnp.float32))
        logarithm_decay = -discrete_step_size * head_decay_rates + decay_spikes
        cumulative_decay = jnp.cumsum(
            logarithm_decay.reshape(blocks, BLOCK, groups_local, per_group), axis=1
        )
        cum_t = cumulative_decay.transpose(0, 2, 3, 1)
        step_t = discrete_step_size.reshape(blocks, BLOCK, groups_local, per_group).transpose(
            0, 2, 3, 1
        )
        heads_x = x_conv.reshape(blocks, BLOCK, groups_local, per_group, HEAD_DIM)
        group_b = b_conv.reshape(blocks, BLOCK, groups_local, STATE)
        group_c = c_conv.reshape(blocks, BLOCK, groups_local, STATE)
        scores = jnp.einsum("ktgn,kugn->kgtu", group_c, group_b, preferred_element_type=jnp.float32)
        causal = jnp.arange(BLOCK)[:, None] >= jnp.arange(BLOCK)[None, :]
        decay_gap = cum_t[..., :, None] - cum_t[..., None, :]
        decay_factor = jnp.where(causal, jnp.exp(jnp.where(causal, decay_gap, 0.0)), 0.0)
        weights = (scores[:, :, None] * decay_factor * step_t[..., None, :]).astype(jnp.bfloat16)
        within = jnp.einsum("kgetu,kugep->ktgep", weights, heads_x, preferred_element_type=jnp.float32)
        block_end = cum_t[..., -1]
        end_weight = jnp.exp(block_end[..., None] - cum_t) * step_t
        scaled_x = (heads_x * end_weight.transpose(0, 3, 1, 2)[..., None]).astype(jnp.bfloat16)
        block_state = jnp.einsum(
            "kugep,kugn->kgepn", scaled_x, group_b, preferred_element_type=jnp.float32
        )

        def local_chain(state_now, current_inputs):
            piece_state, piece_fall = current_inputs
            return (state_now * jnp.exp(piece_fall)[..., None, None] + piece_state, state_now)

        final_state, local_entering = lax.scan(
            local_chain, jnp.zeros(block_state.shape[1:], jnp.float32), (block_state, block_end)
        )
        log_total = jnp.sum(block_end, axis=0)
        prefix_log = jnp.cumsum(block_end, axis=0) - block_end
        log_before, state_before = entering_2(
            (log_total, final_state),
            "sp",
            join_states,
            (jnp.zeros_like(log_total), jnp.zeros_like(final_state)),
        )
        entering = (local_entering + jnp.exp(prefix_log)[..., None, None] * state_before[None]).astype(
            jnp.bfloat16
        )
        carried_out = jnp.einsum(
            "ktgn,kgepn->ktgep", group_c, entering, preferred_element_type=jnp.float32
        )
        carried_out = carried_out * jnp.exp(cumulative_decay)[..., None]
        mixed_ssd = (within + carried_out).reshape(tok_rows, inner_local) * jax.nn.silu(
            output_gate_rows.astype(jnp.float32)
        )
        grouped = mixed_ssd.reshape(tok_rows, groups_local, inner_local // groups_local)
        normed = grouped * lax.rsqrt(jnp.mean(grouped * grouped, axis=-1, keepdims=True) + eps)
        ssd_out = (normed.reshape(tok_rows, inner_local) * gain_ssd.astype(jnp.float32)).astype(
            jnp.bfloat16
        )
        positions = (seq_index * tok_rows + jnp.arange(tok_rows, dtype=jnp.int32)).astype(jnp.float32)
        group_ids = core_index * groups_pool + jnp.arange(pool_local, dtype=jnp.int32) // POOL_GROUP
        pool_out = pool_mix(pooling_rows, prior_pool, positions, group_ids, weight_pool, gain_pool)
        channels = jnp.concatenate([ssd_out, pool_out], axis=1)
    else:
        rates = lax.dynamic_slice_in_dim(logarithm_rates, core_index * heads_local, heads_local, 0)
        group_ids = core_index * groups_pool + jnp.arange(pool_local, dtype=jnp.int32) // POOL_GROUP
        reach = jnp.left_shift(jnp.int32(2), group_ids).astype(jnp.float32)
        bias = jnp.concatenate([bias_b, jnp.zeros_like(bias_b)])
        whole_columns, channels = mixed_and_gathered(
            own_columns,
            (
                head_channel_rows,
                output_gate_rows,
                jnp.concatenate([input_projection_rows, output_projection_rows], axis=1),
                step_size_rows,
                step_size_rows.T,
                decay_spikes,
                decay_spikes.T,
                rates[None],
                rates[:, None],
                taps_x,
                jnp.concatenate([taps_b, taps_c], axis=1),
                bias[None],
                gain_ssd[None],
                pooling_rows,
                weight_pool,
                gain_pool[None],
                reach[None],
                jnp.pad(prior, ((tail - pool_tail, 0), (0, 0))),
            ),
            tail,
        )
    half_width = D // core_count
    gain_out = lax.dynamic_slice_in_dim(
        output_norm_gain, core_index * half_width, half_width, 0
    ).astype(jnp.float32)
    partial = jnp.dot(channels, whole_columns, preferred_element_type=jnp.float32).astype(
        jnp.bfloat16
    )
    own_half = lax.dynamic_slice_in_dim(partial, core_index * half_width, half_width, 1).astype(
        jnp.float32
    )
    for hop in range(1, core_count):
        target = lax.rem(core_index + hop, core_count)
        leaving = lax.dynamic_slice_in_dim(partial, target * half_width, half_width, 1)
        route = [(i, (i + hop) % core_count) for i in range(core_count)]
        own_half = own_half + lax.ppermute(leaving, "tp", route).astype(jnp.float32)
    row_squares = lax.psum(jnp.sum(own_half * own_half, axis=1), "tp")
    result = own_half * lax.rsqrt(row_squares / D + eps)[:, None] * gain_out
    return result.astype(jnp.bfloat16)[None]


def solution(mesh):
    in_specs = (
        P("fs", "sp", "tp"),
        P("fs", "sp", "tp"),
        P("fs", "sp", "tp"),
        P("fs", "sp", "tp"),
        P("fs", "sp", "tp"),
        P("fs", "sp", "tp"),
        P(),
        P(),
        P(),
        P(),
        P(),
        P(),
        P("fs", "sp", "tp"),
        P(),
        P(),
        P("tp", ("sp", "fs")),
        P("tp", ("sp", "fs")),
        P(),
    )
    out_specs = P("fs", "sp", "tp")
    return jax.shard_map(body, mesh=mesh, in_specs=in_specs, out_specs=out_specs, check_vma=False)
```
